32 devices in a mesh: sp: 16 (over z, y, x), tp: 2 (over core).
Axes of the slice: x: 2, y: 2, z: 4, core: 2. Of those that a mesh axis runs over, the one named last changes fastest.
Arguments:
- residual: bfloat16 [2048, 2048], P('sp'), may hold values from -6 to 6
- query_proj: bfloat16 [2048, 1024], P('sp', 'tp'), may hold values from -6 to 6
- key_proj: bfloat16 [2048, 1024], P('sp', 'tp'), may hold values from -6 to 6
- value_proj: bfloat16 [2048, 2048], P('sp', 'tp'), may hold values from -6 to 6
- out_gate: bfloat16 [2048, 2048], P('sp', 'tp'), may hold values from -6 to 6
- log_decay: float32 [2048, 1024], P('sp', 'tp'), may hold values from -1 to 0
- doc_ids: int32 [2048], P('sp'), may hold values from 0 to 3, never falling along the last dimension, each value on 1 to 1536 neighbouring positions
- head_gain: float32 [8, 256], P('tp'), may hold values from 0.1 to 1.9
- w_out: bfloat16 [2048, 2048], P('tp'), may hold values from -0.125 to 0.125
- ffn_gain: float32 [2048], replicated, may hold values from 0.1 to 1.9
- w_gate: bfloat16 [2048, 5120], P('sp', 'tp'), may hold values from -0.125 to 0.125
- w_value: bfloat16 [2048, 5120], P('sp', 'tp'), may hold values from -0.125 to 0.125
- w_down_t: bfloat16 [2048, 5120], P('sp', 'tp'), may hold values from -0.078125 to 0.078125
- conv_taps: float32 [3, 2, 5120], P(None, None, 'tp'), may hold values from -3.5 to 3.5
- conv_bias: float32 [2, 5120], P(None, 'tp'), may hold values from -3 to 3
Outputs:
- result: bfloat16 [2048, 2048], P('sp')
The draws below stay inside these ranges and needn't reach their ends.
Inputs may be any that keep to these rules, and one draw needn't show every extreme that they name: `doc_ids`: document numbers never fall along the sequence; each document holds 1 to 1536 positions, and one holds exactly 1536.
All inputs are finite; a program needn't handle non-finite values.
Results may differ from the reference program's by a relative error of at most 0.017.
Values may be sent and summed in bfloat16 or wider, within the bound.
A program may use at most 128 MiB of HBM per device.

```python
import math
import jax
import jax.numpy as jnp
import numpy as np
from jax import lax

D = 2048
H = 8
DK = 128
DV = 256
FF = 5120
BLOCK = 64
SPAN_LENGTH = 2048
GROUPS = 2
DOCS = 4
DOC_MOST = 1536


def draw_log_decay(key, part):
    packed_texts_batch = jax.random.split(key, 6)
    feature_dimension = H * DK
    slow_share = 0.5
    slow_heads = jax.random.uniform(packed_texts_batch[0], (H,), jnp.float32) < slow_share
    slow_chan = jnp.repeat(slow_heads, DK)
    channel = jnp.exp(jax.random.uniform(packed_texts_batch[1], (feature_dimension,), jnp.float32, -0.7, 0.7))
    fading_speed_reference = jnp.where(slow_chan, 0.7 / SPAN_LENGTH, 1.0 / 40.0) * channel
    segment_fade_multiplier = jnp.exp(jax.random.uniform(packed_texts_batch[2], (SPAN_LENGTH // BLOCK, 1), jnp.float32, -0.7, 0.7))
    segment_fade_multiplier = jnp.repeat(segment_fade_multiplier, BLOCK, axis=0)
    approximate_guess = jax.random.uniform(packed_texts_batch[3], (SPAN_LENGTH, feature_dimension), jnp.float32, 0.5, 1.5)
    spots = jax.random.randint(packed_texts_batch[4], (3,), 0, SPAN_LENGTH)
    removed_elements = jnp.any(jnp.arange(SPAN_LENGTH)[:, None] == spots[None, :], axis=1)
    word_piece_group = jnp.log(jax.random.uniform(packed_texts_batch[5], (SPAN_LENGTH, feature_dimension), jnp.float32, 0.6, 0.85))
    return -fading_speed_reference * segment_fade_multiplier * approximate_guess + jnp.where(removed_elements[:, None], word_piece_group, 0.0)


def block_scale(stream_key, extent, cuts, low, high):
    def one(axis_at, shards_of):
        draws = jax.random.uniform(jax.random.fold_in(jax.random.fold_in(stream_key, 6), axis_at), (shards_of,), jnp.float32, low / len(cuts), high / len(cuts))
        return jnp.repeat(jnp.exp(draws), extent[axis_at] // shards_of).reshape((-1,) + (1,) * (len(extent) - axis_at - 1))

    loudness = one(*cuts[0])
    for cut in cuts[1:]:
        loudness = loudness * one(*cut)
    return loudness


def profile(number_of, total, reach, slope):
    portions = [(1 << 20) // math.isqrt(standing ** slope) + 1 for standing in range(2, number_of + 1)]
    rest, holding = total - reach - (number_of - 1), [1] * (number_of - 1)
    while rest > 0:
        movable = [i for i in range(number_of - 1) if holding[i] < reach]
        mass, left = sum([portions[i] for i in movable]), rest
        for i in movable:
            extra = min(reach - holding[i], max(1, left * portions[i] // mass), rest)
            holding[i] = holding[i] + extra
            rest = rest - extra
    return np.array([reach] + holding)


def uneven(rng, amount, total, bound, slope):
    if amount == 2:
        one = jax.random.randint(rng, (), max(1, total - bound), min(bound, total - 1) + 1)
        return jnp.stack([one, total - one])
    lengths = jnp.asarray(profile(amount, total, bound, slope), jnp.int32)
    pairs = (amount - 1) // 2
    source_of, taker = lengths[1:1 + 2 * pairs:2], lengths[2:2 + 2 * pairs:2]
    slack = jnp.minimum(source_of - 1, bound - taker)
    passed = jax.random.randint(jax.random.fold_in(rng, 1), (pairs,), 0, 1 << 20) % (slack + 1)
    lengths = lengths.at[1:1 + 2 * pairs:2].set(source_of - passed).at[2:2 + 2 * pairs:2].set(taker + passed)
    return lengths[jax.random.permutation(jax.random.fold_in(rng, 2), amount)]


def centred(rng, shape, scale, most, cuts=(), held_as=jnp.bfloat16):
    values = jax.random.normal(rng, shape, jnp.float32) * scale
    if len(cuts) > 0:
        values = block_scale(rng, shape, cuts, -0.22, 0.18) * values
    return jnp.clip(values, min=-most, max=most).astype(held_as)


def setup_inputs(seed: int = 0) -> dict:
    arg_keys = jax.random.split(jax.random.key(seed), 16)
    residual = centred(arg_keys[0], (SPAN_LENGTH, D), 1.0, 6.0, ((0, 16),))
    query_proj = centred(arg_keys[1], (SPAN_LENGTH, H * DK), 1.0, 6.0, ((0, 16), (1, 2)))
    key_proj = centred(arg_keys[2], (SPAN_LENGTH, H * DK), 1.0, 6.0, ((0, 16), (1, 2)))
    value_proj = centred(arg_keys[3], (SPAN_LENGTH, H * DV), 1.0, 6.0, ((0, 16), (1, 2)))
    out_gate = centred(arg_keys[4], (SPAN_LENGTH, H * DV), 1.0, 6.0, ((0, 16), (1, 2)))
    log_decay = draw_log_decay(jax.random.fold_in(arg_keys[15], 71), 0)
    doc_ids = jnp.searchsorted(jnp.cumsum(uneven(arg_keys[6], DOCS, SPAN_LENGTH, DOC_MOST, 0)), jnp.arange(SPAN_LENGTH), side="right").astype(jnp.int32)
    head_gain = jnp.clip(1.0 + 0.18 * jax.random.normal(arg_keys[7], (H, DV), jnp.float32), 0.1, 1.9)
    w_out = centred(arg_keys[8], (H * DV, D), (H * DV) ** -0.5, 0.125, ((0, 2),))
    ffn_gain = jnp.clip(1.0 + 0.18 * jax.random.normal(arg_keys[9], (D,), jnp.float32), 0.1, 1.9)
    w_gate = centred(arg_keys[10], (D, FF), D ** -0.5, 0.125, ((0, 16), (1, 2)))
    w_value = centred(arg_keys[11], (D, FF), D ** -0.5, 0.125, ((0, 16), (1, 2)))
    w_down_t = centred(arg_keys[12], (D, FF), FF ** -0.5, 0.078125, ((0, 16), (1, 2)))
    conv_taps = centred(arg_keys[13], (3, 2, FF), 3 ** -0.5, 3.5, ((2, 2),), jnp.float32)
    conv_bias = centred(arg_keys[14], (2, FF), 0.5, 3.0, ((1, 2),), jnp.float32)
    return {"residual": residual, "query_proj": query_proj, "key_proj": key_proj, "value_proj": value_proj, "out_gate": out_gate, "log_decay": log_decay, "doc_ids": doc_ids, "head_gain": head_gain, "w_out": w_out, "ffn_gain": ffn_gain, "w_gate": w_gate, "w_value": w_value, "w_down_t": w_down_t, "conv_taps": conv_taps, "conv_bias": conv_bias}


EPS = 1e-06

def mix_positions(projected, doc_ids, conv_taps, conv_bias, branch_idx):
    values = projected.astype(jnp.float32)
    lag_one = jnp.pad(values, ((1, 0), (0, 0)))[:-1]
    lag_two = jnp.pad(values, ((2, 0), (0, 0)))[:-2]
    doc_one = jnp.pad(doc_ids, (1, 0), constant_values=-1)[:-1]
    doc_two = jnp.pad(doc_ids, (2, 0), constant_values=-1)[:-2]
    mask_one = (doc_one == doc_ids).astype(jnp.float32)[:, None]
    mask_two = (doc_two == doc_ids).astype(jnp.float32)[:, None]
    return conv_bias[branch_idx] + conv_taps[2, branch_idx] * values + conv_taps[1, branch_idx] * lag_one * mask_one + conv_taps[0, branch_idx] * lag_two * mask_two

def reference(residual, query_proj, key_proj, value_proj, out_gate, log_decay, doc_ids, head_gain, w_out, ffn_gain, w_gate, w_value, w_down_t, conv_taps, conv_bias):
    highest_precision = lax.Precision.HIGHEST
    number = SPAN_LENGTH // BLOCK

    def blocks(source, feature_dimension):
        return source.astype(jnp.float32).reshape(number, BLOCK, H, feature_dimension).transpose(0, 2, 1, 3)
    q_blocks = blocks(query_proj, DK) * DK ** (-0.5)
    k_blocks = blocks(key_proj, DK)
    v_blocks = blocks(value_proj, DV)
    g_blocks = blocks(log_decay, DK)
    d_blocks = doc_ids.reshape(number, BLOCK)
    causal = jnp.tril(jnp.ones((BLOCK, BLOCK), bool))

    def advance(carried_in, inputs):
        state_sequence, before = carried_in
        current_queries, current_keys, current_values, g_now, d_now = inputs
        cumulative_log_decay = jnp.cumsum(g_now, axis=1)
        keep_mask = (d_now == before).astype(jnp.float32)
        carried_state = jnp.einsum('obl,olx->obx', current_queries * jnp.exp(cumulative_log_decay), state_sequence, precision=highest_precision)
        carried_state = carried_state * keep_mask[None, :, None]
        same_doc = causal & (d_now[:, None] == d_now[None, :])
        log_gap = cumulative_log_decay[:, :, None, :] - cumulative_log_decay[:, None, :, :]
        weight = jnp.where(same_doc[None, :, :, None], jnp.exp(jnp.minimum(log_gap, 0.0)), 0.0)
        scores = jnp.einsum('htk,hsk,htsk->hts', current_queries, current_keys, weight, precision=highest_precision)
        within = jnp.einsum('hts,hsv->htv', scores, current_values, precision=highest_precision)
        total_log_decay = cumulative_log_decay[:, -1, :]
        trailing_mask = (d_now == d_now[-1]).astype(jnp.float32)
        initial_state = jnp.einsum('cxu,cxg->cug', current_keys * jnp.exp(total_log_decay[:, None, :] - cumulative_log_decay) * trailing_mask[None, :, None], current_values, precision=highest_precision)
        state_sequence = state_sequence * (jnp.exp(total_log_decay) * keep_mask[-1])[:, :, None] + initial_state
        return ((state_sequence, d_now[-1]), carried_state + within)
    start = (jnp.zeros((H, DK, DV), jnp.float32), jnp.array(-1, jnp.int32))
    _, block_out = lax.scan(advance, start, (q_blocks, k_blocks, v_blocks, g_blocks, d_blocks))
    head_out = block_out.transpose(0, 2, 1, 3).reshape(SPAN_LENGTH, H, DV)
    head_out = head_out * lax.rsqrt(lax.optimization_barrier(jnp.mean(head_out * head_out, axis=-1, keepdims=True)) + EPS) * head_gain
    mixed_heads = (head_out.reshape(SPAN_LENGTH, H * DV) * jax.nn.silu(out_gate.astype(jnp.float32))).astype(jnp.bfloat16)
    group_cols = H * DV // GROUPS
    attn_sum = jnp.zeros((SPAN_LENGTH, D), jnp.float32)
    for member in range(GROUPS):
        term = jnp.dot(mixed_heads[:, member * group_cols:(member + 1) * group_cols], w_out[member * group_cols:(member + 1) * group_cols], preferred_element_type=jnp.float32)
        attn_sum = attn_sum + term.astype(jnp.bfloat16).astype(jnp.float32)
    stream = (residual.astype(jnp.float32) + attn_sum).astype(jnp.bfloat16)
    stream_f = stream.astype(jnp.float32)
    normed = (stream_f * lax.rsqrt(lax.optimization_barrier(jnp.mean(stream_f * stream_f, axis=-1, keepdims=True)) + EPS) * ffn_gain).astype(jnp.bfloat16)
    gate_up = jnp.dot(normed, w_gate, preferred_element_type=jnp.float32).astype(jnp.bfloat16)
    value_up = jnp.dot(normed, w_value, preferred_element_type=jnp.float32).astype(jnp.bfloat16)
    gate_mix = mix_positions(gate_up, doc_ids, conv_taps, conv_bias, 0)
    value_mix = mix_positions(value_up, doc_ids, conv_taps, conv_bias, 1)
    hidden = (jax.nn.silu(gate_mix) * value_mix).astype(jnp.bfloat16)
    group_units = FF // GROUPS
    ffn_sum = jnp.zeros((SPAN_LENGTH, D), jnp.float32)
    for member in range(GROUPS):
        cols = slice(member * group_units, (member + 1) * group_units)
        term = lax.dot_general(hidden[:, cols], w_down_t[:, cols], (((1,), (1,)), ((), ())), preferred_element_type=jnp.float32)
        ffn_sum = ffn_sum + term.astype(jnp.bfloat16).astype(jnp.float32)
    return (stream_f + ffn_sum).astype(jnp.bfloat16)
```

```python
import functools

import jax
import jax.numpy as jnp
from jax import lax
from jax.experimental import pallas as pl
from jax.experimental.pallas import tpu as pltpu
from jax.sharding import PartitionSpec as P

EPS = 1e-06
VMEM = pl.BlockSpec(memory_space=pltpu.VMEM)
HIGH = lax.Precision.HIGHEST
BF = jnp.bfloat16
F32 = jnp.float32


def plane_count(positions, hidden):
    return max(b for b in (1, 2, 4) if positions % b == 0 and (hidden // b) % 128 == 0)


def nt(a, b):
    return lax.dot_general(a, b, (((1,), (1,)), ((), ())), preferred_element_type=F32)


def tn(a, b):
    return lax.dot_general(a, b, (((0,), (0,)), ((), ())), preferred_element_type=F32)


def local_kernel(heads, q_ref, k_ref, v_ref, g_ref, dcol_ref, drow_ref, o_ref, s_ref, qd_ref, cum_ref):
    rows = q_ref.shape[0]
    dk = q_ref.shape[1] // heads
    dv = v_ref.shape[1] // heads
    half = rows // 2
    t = lax.broadcasted_iota(jnp.int32, (rows, rows), 0)
    s = lax.broadcasted_iota(jnp.int32, (rows, rows), 1)
    tril = (t >= s).astype(F32)
    cum_ref[...] = jnp.dot(tril, g_ref[...], precision=HIGH, preferred_element_type=F32)
    dcol = dcol_ref[...]
    allowed = (t >= s) & (dcol == drow_ref[...])
    tail = (dcol == dcol_ref[rows - 1:rows, :]).astype(F32)
    scale = dk ** -0.5
    for h in range(heads):
        kc = pl.ds(h * dk, dk)
        vc = pl.ds(h * dv, dv)
        cum = cum_ref[:, kc]
        q = q_ref[:, kc].astype(F32) * scale
        k = k_ref[:, kc].astype(F32)
        v = v_ref[:, vc]
        total = cum[rows - 1:rows, :]
        qd_ref[:, kc] = (q * jnp.exp(cum)).astype(BF)
        s_ref[kc, :] = tn((k * jnp.exp(total - cum) * tail).astype(BF), v).astype(BF)
        edge = cum[half - 1:half, :]
        for part in range(2):
            rs = slice(part * half, (part + 1) * half)
            mid = cum[part * half + half // 2 - 1:part * half + half // 2, :]
            qs = (q[rs] * jnp.exp(cum[rs] - mid)).astype(BF)
            ks = (k[rs] * jnp.exp(mid - cum[rs])).astype(BF)
            a = jnp.where(allowed[rs, rs], nt(qs, ks), 0.0).astype(BF)
            o = jnp.dot(a, v[rs], preferred_element_type=F32)
            if part == 1:
                qx = (q[rs] * jnp.exp(cum[rs] - edge)).astype(BF)
                kx = (k[:half] * jnp.exp(edge - cum[:half])).astype(BF)
                x = jnp.where(allowed[rs, :half], nt(qx, kx), 0.0).astype(BF)
                o = o + jnp.dot(x, v[:half], preferred_element_type=F32)
            o_ref[rs, vc] = o


def out_kernel(heads, o_ref, qd_ref, p_ref, reach_ref, gate_ref, gain_ref, w_ref, out_ref, mixed):
    dk = qd_ref.shape[1] // heads
    dv = o_ref.shape[1] // heads
    for h in range(heads):
        kc = pl.ds(h * dk, dk)
        vc = pl.ds(h * dv, dv)
        carried = jnp.dot(qd_ref[:, kc], p_ref[kc, :], preferred_element_type=F32)
        head = o_ref[:, vc] + carried * reach_ref[...]
        head = head * lax.rsqrt(jnp.mean(head * head, axis=-1, keepdims=True) + EPS) * gain_ref[h:h + 1, :]
        gate = gate_ref[:, vc].astype(F32)
        mixed[:, vc] = (head * gate / (1.0 + jnp.exp(-gate))).astype(BF)
    out_ref[...] = jnp.dot(mixed[...], w_ref[...], preferred_element_type=F32).astype(BF)


def rotate(value, count, stride_in, size, steps):
    perm = []
    for i in range(count):
        d = (i // stride_in) % size
        perm.append((i, i + (((d + steps) % size) - d) * stride_in))
    return lax.ppermute(value, "sp", perm)


def swap(value):
    n = lax.axis_size("tp")
    return [lax.ppermute(value, "tp", [(i, (i + k) % n) for i in range(n)]) for k in range(1, n)]


def tp_gather(value):
    n = lax.axis_size("tp")
    if n != 2:
        return lax.all_gather(value, "tp", axis=0)
    (other,) = swap(value)
    first = lax.axis_index("tp") == 0
    return jnp.stack([jnp.where(first, value, other), jnp.where(first, other, value)])


def tp_scatter(value):
    n = lax.axis_size("tp")
    if n != 2:
        return lax.psum_scatter(value, "tp", scatter_dimension=0, tiled=False).astype(F32)
    c = lax.axis_index("tp")
    give = lax.dynamic_index_in_dim(value, 1 - c, 0, False)
    keep = lax.dynamic_index_in_dim(value, c, 0, False)
    return keep.astype(F32) + swap(give)[0].astype(F32)


def ordered(own, received, place, size):
    buf = jnp.zeros((size,) + own.shape, own.dtype)
    buf = lax.dynamic_update_index_in_dim(buf, own, place, 0)
    for k, item in enumerate(received, 1):
        buf = lax.dynamic_update_index_in_dim(buf, item, (place - k) % size, 0)
    return buf


def plane_gather(block, count, m, r, groups):
    b, depth, columns = block.shape
    if m != 4 or b % 2:
        got = lax.all_gather(block, "sp", axis=0, axis_index_groups=groups)
        return got.transpose(1, 0, 2, 3).reshape(b * m * depth, columns)
    half = b // 2
    near = rotate(block, count, 1, 2, 1)
    far = rotate(block, count, 2, 2, 1)
    diag_top = rotate(near[:half], count, 2, 2, 1)
    diag_low = rotate(far[half:], count, 1, 2, 1)
    x, y = r % 2, r // 2
    buf = jnp.zeros((b, m, depth, columns), block.dtype)

    def put(buf, item, first, i, j):
        return lax.dynamic_update_slice(buf, item[:, None], (first, 2 * j + i, 0, 0))

    buf = put(buf, block, 0, x, y)
    buf = put(buf, near, 0, 1 - x, y)
    buf = put(buf, far, 0, x, 1 - y)
    buf = put(buf, diag_top, 0, 1 - x, 1 - y)
    buf = put(buf, diag_low, half, 1 - x, 1 - y)
    return buf.reshape(b * m * depth, columns)


def per_device(residual, query_proj, key_proj, value_proj, out_gate, log_decay, doc_ids, head_gain,
               w_out, ffn_gain, w_gate, w_value, w_down_t, conv_taps, conv_bias):
    count = lax.axis_size("sp")
    rows = doc_ids.shape[0]
    heads = head_gain.shape[0]
    dk = query_proj.shape[1] // heads
    dv = value_proj.shape[1] // heads
    depth, hidden_here = w_gate.shape
    width = residual.shape[1]
    if one_kernel(count, lax.axis_size("tp"), rows, heads, dk, dv, width, hidden_here):
        return fused(residual, query_proj, key_proj, value_proj, out_gate, log_decay, doc_ids, head_gain,
                     w_out, ffn_gain, w_gate, w_value, w_down_t, conv_taps, conv_bias)
    b = plane_count(count, hidden_here)
    m = count // b
    fc = hidden_here // b
    place = lax.axis_index("sp")
    z, r = place // m, place % m
    groups = [[g * m + i for i in range(m)] for g in range(b)]

    note = jnp.concatenate([jnp.sum(log_decay, axis=0), doc_ids.astype(F32)])
    if b == 1:
        notes = lax.all_gather(note, "sp", axis=0)
    else:
        note = note[None]
        plane = ordered(note, [rotate(note, count, 1, m, k) for k in range(1, m)], r, m)
        notes = ordered(plane, [rotate(plane, count, m, b, k) for k in range(1, b)], z, b)
        notes = notes.reshape(count, -1)
    w_gate, w_value, notes = lax.optimization_barrier((w_gate, w_value, notes))

    def chunk(w, j):
        return lax.dynamic_slice_in_dim(w, j * fc, fc, 1)

    def exchange(pick):
        received = [rotate(pick((z + k) % b), count, m, b, k) for k in range(1, b)]
        block = ordered(pick(z), received, z, b)
        return plane_gather(block, count, m, r, groups)

    up_w = exchange(lambda j: jnp.concatenate([chunk(w_gate, j), chunk(w_value, j)], axis=1))

    totals, docs = notes[:, :heads * dk], notes[:, heads * dk:]
    first, last = docs[:, 0], docs[:, -1]
    steps = jnp.arange(count)

    o_local, state, q_dec = pl.pallas_call(
        functools.partial(local_kernel, heads),
        out_shape=(
            jax.ShapeDtypeStruct((rows, heads * dv), F32),
            jax.ShapeDtypeStruct((heads * dk, dv), BF),
            jax.ShapeDtypeStruct((rows, heads * dk), BF),
        ),
        in_specs=[VMEM] * 6,
        out_specs=(VMEM,) * 3,
        scratch_shapes=[pltpu.VMEM((rows, heads * dk), F32)],
        cost_estimate=pl.CostEstimate(flops=10**9, bytes_accessed=3 * 10**6, transcendentals=0),
    )(query_proj, key_proj, value_proj, log_decay, doc_ids[:, None], doc_ids[None, :])

    if b > 1:
        state, _ = lax.optimization_barrier((state, plane))

    def weight(source, until):
        inside = (steps > source) & (steps < until)
        return jnp.exp(jnp.sum(jnp.where(inside[:, None], totals, 0.0), axis=0))

    my_first = first[place]
    if b == 1:
        all_states = lax.all_gather(state, "sp", axis=0)

        def add(i, acc):
            live = (i < place) & (last[i] == my_first)
            scale = jnp.where(live, weight(i, place), 0.0)
            return acc + scale[:, None] * all_states[i].astype(F32)

        prefix = lax.fori_loop(0, count, add, jnp.zeros(state.shape, F32))
    else:
        near = [state] + [rotate(state, count, 1, m, k) for k in range(1, m)]
        end = (z + 1) * m
        start = z * m
        rows_of = []
        for k in range(1, m):
            source = start + (r - k) % m
            rows_of.append((source, place, (source < place) & (last[source] == my_first)))
        for k in range(m):
            source = start + (r - k) % m
            rows_of.append((source, end, last[source] == last[end - 1]))
        for k in range(1, b):
            source = jnp.maximum(z - k + 1, 0) * m - 1
            rows_of.append((source, start, (z >= k) & (last[source] == first[start])))
        rows_of.append((start - 1, place, first[start] == my_first))
        sources, untils, lives = (jnp.stack(col)[:, None] for col in zip(*rows_of))
        inside = ((steps > sources) & (steps < untils)).astype(F32)
        gaps = lax.dot_general(totals, inside, (((0,), (1,)), ((), ())), precision=HIGH,
                               preferred_element_type=F32)
        scales = jnp.where(lives[:, 0], jnp.exp(jnp.minimum(gaps, 0.0)), 0.0)
        pick_scale = lambda i: scales[:, i:i + 1]
        prefix = sum(pick_scale(k - 1) * near[k].astype(F32) for k in range(1, m))
        plane_end = sum(pick_scale(m - 1 + k) * near[k].astype(F32) for k in range(m)).astype(BF)
        whole = sum(
            pick_scale(2 * m - 2 + k)
            * lax.ppermute(plane_end, "sp", [(i, i + k * m) for i in range(count - k * m)]).astype(F32)
            for k in range(1, b)
        )
        prefix += pick_scale(2 * m - 2 + b) * whole

    prefix = prefix.astype(BF)
    w_down_t, prefix = lax.optimization_barrier((w_down_t, prefix))
    down_w = exchange(lambda j: chunk(w_down_t, j))

    own_docs = doc_ids.astype(F32)
    prev_last = jnp.where(place > 0, last[place - 1], -1.0)
    reach_rows = ((own_docs == my_first) & (prev_last == my_first)).astype(F32)[:, None]
    attn = pl.pallas_call(
        functools.partial(out_kernel, heads),
        out_shape=jax.ShapeDtypeStruct((rows, width), BF),
        in_specs=[VMEM] * 7,
        out_specs=VMEM,
        scratch_shapes=[pltpu.VMEM((rows, heads * dv), BF)],
        cost_estimate=pl.CostEstimate(flops=10**9, bytes_accessed=6 * 10**6, transcendentals=0),
    )(o_local, q_dec, prefix, reach_rows, out_gate, head_gain, w_out)

    tp = lax.axis_size("tp")
    share = rows // tp
    core = lax.axis_index("tp")
    attn_sum = tp_scatter(attn.reshape(tp, share, width))
    own_rows = lax.dynamic_slice_in_dim(residual, core * share, share, 0)
    stream = (own_rows.astype(F32) + attn_sum).astype(BF)
    stream_f = stream.astype(F32)
    normed = (stream_f * lax.rsqrt(jnp.mean(stream_f * stream_f, axis=-1, keepdims=True) + EPS) * ffn_gain).astype(BF)
    blocks = ordered(normed, [rotate(normed, count, m, b, k) for k in range(1, b)], z, b)
    full = tp_gather(blocks).transpose(1, 0, 2, 3).reshape(b * rows, width)
    ups = jnp.dot(full, up_w, preferred_element_type=F32).astype(BF).reshape(b, rows, 2 * fc)

    tails = rotate(ups[:, -2:], count, 1, m, 1)
    lead = jnp.where(r == 0, jnp.roll(tails, 1, axis=0), tails)
    ext = jnp.concatenate([lead, ups], axis=1).astype(F32)
    at = jnp.arange(b) * m + r
    block_docs = docs[at]
    prev = jnp.where((at > 0)[:, None], docs[(at - 1) % count][:, -2:], -1.0)
    doc_ext = jnp.concatenate([prev, block_docs], axis=1)
    one = (doc_ext[:, 1:-1] == block_docs).astype(F32)[:, :, None]
    two = (doc_ext[:, :-2] == block_docs).astype(F32)[:, :, None]
    taps = lax.dynamic_slice_in_dim(conv_taps, z * fc, fc, 2).reshape(3, 2 * fc)
    bias = lax.dynamic_slice_in_dim(conv_bias, z * fc, fc, 1).reshape(2 * fc)
    mix = bias + taps[2] * ext[:, 2:] + taps[1] * ext[:, 1:-1] * one + taps[0] * ext[:, :-2] * two
    gate_mix, value_mix = mix[..., :fc], mix[..., fc:]
    hidden = (jax.nn.silu(gate_mix) * value_mix).astype(BF).reshape(b * rows, fc)
    partial = nt(hidden, down_w).astype(BF)

    partial = partial.reshape(b, tp, share, width).transpose(1, 0, 2, 3)
    pair = tp_scatter(partial).astype(BF)
    total = lax.dynamic_index_in_dim(pair, z, 0, False).astype(F32)
    for k in range(1, b):
        total += rotate(lax.dynamic_index_in_dim(pair, (z + k) % b, 0, False), count, m, b, k).astype(F32)
    finished = (stream_f + total).astype(BF)
    return tp_gather(finished).reshape(rows, width)


MESH = pl.DeviceIdType.MESH


def fused_kernel(cfg, q_hbm, k_hbm, v_hbm, g_hbm, gate_hbm, res_hbm, wo_hbm, wg_hbm, wv_hbm, wd_hbm,
                 doc_ref, gain_ref, fgain_ref, taps_ref, bias_ref, out_hbm,
                 qb, kb, vb, gb, gateb, resb, wo, ugv, ud, cum_ref, notes, qd, o_ref, s_own, s_x, t2, s_y, e_in, e_out, pref,
                 acc, a_own, a_peer, stream_ref, nf, ups, tail_s, tail_r, masks, hid, pb, pr, qq, rb, fb,
                 loc, n_s, n_r, wz_s, w_r, wx_s, wy_s, wd_s, sx_s, sx_r, sy_s, sy_r, sz_s, sz_r, ap_s, ap_r,
                 nz_s, nz_r, nd_s, nd_r, tl_s, tl_r, dp_s, dp_r, rs_s, rs_r, f_s, f_r):
    heads, dk, dv, rows, width, fc, count = cfg
    b = m = 4
    half, share, quarter = rows // 2, rows // 2, width // b
    hbm_w = (wg_hbm, wv_hbm, wd_hbm)
    p, c = lax.axis_index("sp"), lax.axis_index("tp")
    z, r = lax.div(p, m), lax.rem(p, m)
    x, y = lax.rem(r, 2), lax.div(r, 2)
    xr, yr = r + 1 - 2 * x, r + 2 - 4 * y
    xn, yn, base = z * m + xr, z * m + yr, z * m
    peer = {"tp": 1 - c}

    def remote(src, dst, ss, rs, dev):
        return pltpu.make_async_remote_copy(src_ref=src, dst_ref=dst, send_sem=ss, recv_sem=rs, device_id=dev,
                                            device_id_type=MESH)

    def at_z(k):
        return lax.rem(z + k, b)

    def blk(i, n):
        return pl.ds(pl.multiple_of(i * n, n), n)

    def w_at(w, i):
        if w == 2:
            return ud.at[blk(i, rows), :]
        return ugv.at[blk(i, rows), pl.ds(w * fc, fc)]

    def w_from(w, zz):
        return hbm_w[w].at[:, pl.ds(pl.multiple_of(zz * fc, 128), fc)]

    local = [pltpu.make_async_copy(src, dst, loc.at[i]) for i, (src, dst) in enumerate([
        (g_hbm, gb), (k_hbm, kb), (v_hbm, vb), (q_hbm, qb), (gate_hbm, gateb),
        (res_hbm.at[blk(c, share), :], resb), (wo_hbm, wo),
        (w_from(0, z), w_at(0, p)), (w_from(1, z), w_at(1, p)), (w_from(2, z), w_at(2, p))])]
    for copy in local:
        copy.start()

    barrier = pltpu.get_barrier_semaphore()
    for k in range(1, count):
        pl.semaphore_signal(barrier, inc=1, device_id={"sp": lax.rem(p + k, count)}, device_id_type=MESH)
    pl.semaphore_signal(barrier, inc=1, device_id=peer, device_id_type=MESH)

    ti = lax.broadcasted_iota(jnp.int32, (rows, rows), 0)
    si = lax.broadcasted_iota(jnp.int32, (rows, rows), 1)
    lower, same = ti >= si, ti == si

    def column(row):
        return jnp.sum(jnp.where(same, row, 0.0), axis=1, keepdims=True)

    drow = doc_ref[...].astype(F32)
    dcol = column(drow)
    allowed = lower & (dcol == drow)
    last_doc = drow[:, rows - 1:rows]
    tail = (dcol == last_doc).astype(F32)
    tril = lower.astype(F32).astype(BF)

    local[0].wait()
    decay = gb[...]
    d1 = decay.astype(BF)
    rest = decay - d1.astype(F32)
    d2 = rest.astype(BF)
    d3 = (rest - d2.astype(F32)).astype(BF)
    dot = functools.partial(jnp.dot, preferred_element_type=F32)
    cum_ref[...] = dot(tril, d1) + (dot(tril, d2) + dot(tril, d3))
    for h in range(heads):
        notes[p, h:h + 1, :] = cum_ref[rows - 1:rows, h * dk:(h + 1) * dk]
    for h in range(heads, 4):
        notes[p, h:h + 1, :] = jnp.zeros((1, dk), F32)
    notes[p, 4:5, :] = drow
    notes[p, 5:6, :] = drow
    notes[p, 6:7, :] = jnp.broadcast_to(last_doc, (1, rows))
    notes[p, 7:8, :] = drow

    @pl.when(z == 0)
    def _():
        e_in[...] = jnp.zeros_like(e_in)

    pl.semaphore_wait(barrier, count)

    def note_copy(k):
        to = lax.rem(p + k, count)
        return remote(notes.at[p], notes.at[p], n_s.at[k], n_r.at[p], {"sp": to})

    for k in range(1, count):
        note_copy(k).start()

    def z_copy(w, k):
        zz = at_z(k)
        return remote(w_from(w, zz), w_at(w, p), wz_s.at[w, k], w_r.at[w, p], {"sp": zz * m + r})

    def near_copies(w, k):
        i = at_z(k) * m + r
        src = w_from(w, z) if k == 0 else w_at(w, i)
        return (remote(src, w_at(w, i), wx_s.at[w, k], w_r.at[w, i], {"sp": xn}),
                remote(src, w_at(w, i), wy_s.at[w, k], w_r.at[w, i], {"sp": yn}))

    def diag_copy(w, k):
        zs = at_z(k)
        even = lax.rem(zs, 2) == 0
        i = zs * m + jnp.where(even, xr, yr)
        return remote(w_at(w, i), w_at(w, i), wd_s.at[w, k], w_r.at[w, i], {"sp": jnp.where(even, yn, xn)})

    def arrived(w, i):
        remote(w_at(w, i), w_at(w, i), wx_s.at[w, 0], w_r.at[w, i], {"sp": xn}).wait_recv()

    def near(w, k):
        if k > 0:
            arrived(w, at_z(k) * m + r)
        for copy in near_copies(w, k):
            copy.start()

    def diag(w, k):
        zs = at_z(k)
        arrived(w, zs * m + jnp.where(lax.rem(zs, 2) == 0, xr, yr))
        diag_copy(w, k).start()

    def settle(w, k):
        zs = at_z(k)
        arrived(w, zs * m + jnp.where(lax.rem(zs, 2) == 0, yr, xr))
        arrived(w, zs * m + 3 - r)

    near_g = near_copies(0, 0)
    near_v = near_copies(1, 0)
    near_g[0].start()
    near_g[1].start()
    near_v[1].start()
    for k in (1, 3, 2):
        z_copy(0, k).start()
    for k in (1, 2, 3):
        @pl.when(at_z(k) < z)
        def _(k=k):
            z_copy(1, k).start()

    local[1].wait()
    local[2].wait()

    def s_copy(h):
        return remote(s_own.at[blk(h, dv), :], s_x.at[blk(h, dv), :], sx_s.at[h], sx_r.at[h], {"sp": xn})

    def t_copy(h):
        return remote(t2.at[blk(h, dv), :], s_y.at[blk(h, dv), :], sy_s.at[h], sy_r.at[h], {"sp": yn})

    def e_copy(h):
        return remote(e_out.at[blk(h, dv), :], e_in.at[blk(h, dv), :], sz_s.at[h], sz_r.at[h],
                      {"sp": jnp.minimum(p + m, count - m + r)})

    for h in range(heads):
        kc, vc = slice(h * dk, (h + 1) * dk), slice(h * dv, (h + 1) * dv)
        cum = cum_ref[:, kc]
        k_end = (kb[:, kc].astype(F32) * jnp.exp(cum[rows - 1:rows, :] - cum) * tail).astype(BF)
        s_own[vc, :] = tn(vb[:, vc], k_end).astype(BF)
        s_copy(h).start()
    near_v[0].start()

    local[3].wait()
    scale = dk ** -0.5
    for h in range(heads):
        kc, vc = slice(h * dk, (h + 1) * dk), slice(h * dv, (h + 1) * dv)
        cum = cum_ref[:, kc]
        q = qb[:, kc].astype(F32) * scale
        k = kb[:, kc].astype(F32)
        v = vb[:, vc]
        qd[:, kc] = (q * jnp.exp(cum)).astype(BF)
        edge = cum[half - 1:half, :]
        for part in range(2):
            rs = slice(part * half, (part + 1) * half)
            mid = cum[part * half + half // 2 - 1:part * half + half // 2, :]
            qs = (q[rs] * jnp.exp(cum[rs] - mid)).astype(BF)
            ks = (k[rs] * jnp.exp(mid - cum[rs])).astype(BF)
            a = jnp.where(allowed[rs, rs], nt(qs, ks), 0.0).astype(BF)
            o = dot(a, v[rs])
            if part == 1:
                qx = (q[rs] * jnp.exp(cum[rs] - edge)).astype(BF)
                kx = (k[:half] * jnp.exp(edge - cum[:half])).astype(BF)
                cross = jnp.where(allowed[rs, :half], nt(qx, kx), 0.0).astype(BF)
                o = o + dot(cross, v[:half])
            o_ref[rs, vc] = o

    for k in range(1, count):
        frm = lax.rem(p + count - k, count)
        remote(notes.at[frm], notes.at[frm], n_s.at[k], n_r.at[frm], {"sp": frm}).wait_recv()

    def last_of(i):
        return notes[i, 6:7, :]

    def weight(source, until, live):
        total = jnp.zeros((8, dk), F32)
        for s in range(count):
            total = total + jnp.where((s > source) & (s < until), notes[s], 0.0)
        total = jnp.exp(jnp.minimum(total, 0.0))
        return jnp.where(live, total, 0.0)

    before = jnp.maximum(p - 1, 0)
    plane_before = jnp.maximum(base - 1, 0)
    pair = p - x
    w_pair = weight(pair, pair + 2, last_of(pair) == last_of(pair + 1))
    w_plane = weight(base + 1, base + m, last_of(base + 1) == last_of(base + 3))
    w_line = weight(base - 1, base + m, (last_of(plane_before) == last_of(base + 3)) & (z > 0))
    w_py = weight(base + 1, p, (last_of(base + 1) == last_of(before)) & (y == 1))
    w_pz = weight(base - 1, p, (last_of(plane_before) == last_of(before)) & (z > 0))
    reach = ((dcol == column(jnp.broadcast_to(notes[before, 6:7, :], (rows, rows)))) & (p > 0)).astype(F32)

    for h in range(heads):
        vc = slice(h * dv, (h + 1) * dv)
        s_copy(h).wait_recv()
        own, got = s_own[vc, :].astype(F32), s_x[vc, :].astype(F32)
        left = jnp.where(x == 0, own, got)
        right = jnp.where(x == 0, got, own)
        t2[vc, :] = (right + left * w_pair[h:h + 1, :]).astype(BF)
        t_copy(h).start()
        pref[vc, :] = jnp.where(x == 1, got, 0.0)

    diag(0, 0)
    for copy in local[4:]:
        copy.wait()

    for h in range(heads):
        kc, vc = slice(h * dk, (h + 1) * dk), slice(h * dv, (h + 1) * dv)
        t_copy(h).wait_recv()
        own, got = t2[vc, :].astype(F32), s_y[vc, :].astype(F32)
        left = jnp.where(y == 0, own, got)
        right = jnp.where(y == 0, got, own)
        plane = right + left * w_plane[h:h + 1, :]

        @pl.when(z > 0)
        def _(h=h):
            e_copy(h).wait_recv()
        enter = e_in[vc, :].astype(F32)
        e_out[vc, :] = (plane + enter * w_line[h:h + 1, :]).astype(BF)

        @pl.when(z < b - 1)
        def _(h=h):
            e_copy(h).start()
        prefix = pref[vc, :] + got * w_py[h:h + 1, :] + enter * w_pz[h:h + 1, :]
        carried = nt(qd[:, kc], prefix.astype(BF))
        head = o_ref[:, vc] + carried * reach
        head = head * lax.rsqrt(jnp.mean(head * head, axis=-1, keepdims=True) + EPS) * gain_ref[h:h + 1, :]
        gate = gateb[:, vc].astype(F32)
        mixed = (head * gate / (1.0 + jnp.exp(-gate))).astype(BF)
        if h == 0:
            acc[...] = dot(mixed, wo[vc, :])
        else:
            acc[...] += dot(mixed, wo[vc, :])
        if h < b - 1:
            near(0, h + 1)
    for k in range(heads, b):
        near(0, k)

    for k in (1, 2, 3):
        @pl.when(at_z(k) > z)
        def _(k=k):
            z_copy(1, k).start()

    a_own[0] = acc[0:share, :].astype(BF)
    a_own[1] = acc[share:rows, :].astype(BF)
    a_copy = remote(a_own.at[1 - c], a_peer, ap_s, ap_r, peer)
    a_copy.start()
    diag(0, 1)

    for zb in range(b):
        at = zb * m + r
        row = notes[at, 4:5, :]
        prow = jnp.where(at > 0, notes[jnp.maximum(at - 1, 0), 4:5, :], -1.0)
        lane = lax.broadcasted_iota(jnp.int32, (1, rows), 1)
        for lag in (1, 2):
            shifted = jnp.where(lane < lag, pltpu.roll(prow, lag, 1), pltpu.roll(row, lag, 1))
            masks[lag - 1, zb] = column((shifted == row).astype(F32))

    a_copy.wait_recv()
    stream = (resb[...].astype(F32) + (a_own[c].astype(F32) + a_peer[...].astype(F32))).astype(BF)
    stream_ref[...] = stream
    stream_f = stream.astype(F32)
    normed = (stream_f * lax.rsqrt(jnp.mean(stream_f * stream_f, axis=-1, keepdims=True) + EPS) * fgain_ref[...]).astype(BF)
    nf[z, c] = normed

    def n_copy(k):
        return remote(nf.at[z, c], nf.at[z, c], nz_s.at[k], nz_r.at[z], {"sp": at_z(k) * m + r})

    def n_pass(k):
        zz = at_z(k)
        return remote(nf.at[zz, c], nf.at[zz, c], nd_s.at[k], nd_r.at[k], peer)

    for k in (2, 1, 3):
        n_copy(k).start()
    n_pass(0).start()

    def n_take(k):
        zz = at_z(k)
        remote(nf.at[zz, c], nf.at[zz, c], nz_s.at[k], nz_r.at[zz], {"sp": zz * m + r}).wait_recv()
        n_pass(k).start()

    diag(0, 2)
    diag(0, 3)
    diag(1, 0)
    for k in (1, 3, 2):
        near(1, k)
    for k in (1, 3, 2):
        z_copy(2, k).start()
    for k in (1, 3, 2):
        diag(1, k)
    near(2, 0)
    for k in (1, 3, 2):
        n_take(k)
    for k in range(b):
        zz = at_z(k)
        remote(nf.at[zz, 1 - c], nf.at[zz, 1 - c], nd_s.at[k], nd_r.at[k], peer).wait_recv()
    for k in range(b):
        settle(0, k)
    for k in range(b):
        settle(1, k)
    diag(2, 0)

    lanes = 256 if (2 * fc) % 256 == 0 else 128

    @pl.loop(0, 2 * fc // lanes)
    def _(j):
        cs = pl.ds(pl.multiple_of(j * lanes, lanes), lanes)
        full = nf[...].reshape(b * rows, width)
        up = dot(full, ugv[:, cs]).astype(BF).astype(F32)
        for zb in range(b):
            ups[zb, 8:8 + rows, cs] = up[zb * rows:(zb + 1) * rows]
            tail_s[2 * zb:2 * zb + 2, cs] = up[(zb + 1) * rows - 2:(zb + 1) * rows]

    tails = remote(tail_s, tail_r, tl_s, tl_r, {"sp": base + lax.rem(r + 1, m)})
    tails.start()
    for k in (1, 3, 2):
        near(2, k)
    tails.wait_recv()
    got = tail_r[...]
    for zb in range(b):
        prev = (zb - 1) % b
        ups[zb, 6:8, :] = jnp.where(r == 0, got[2 * prev:2 * prev + 2], got[2 * zb:2 * zb + 2])

    off = pl.multiple_of(z * fc, 128)
    taps = [taps_ref[i, :, pl.ds(off, fc)] for i in range(3)]
    bias = bias_ref[:, pl.ds(off, fc)]

    @pl.loop(0, b)
    def _(zb):
        one, two = masks[0, zb], masks[1, zb]

        def mix(w):
            cols = slice(w * fc, (w + 1) * fc)
            t = [tap[w:w + 1] for tap in taps]
            return (bias[w:w + 1] + t[2] * ups[zb, 8:8 + rows, cols] + t[1] * ups[zb, 7:7 + rows, cols] * one
                    + t[0] * ups[zb, 6:6 + rows, cols] * two)

        gate_mix, value_mix = mix(0), mix(1)
        hid[blk(zb, rows), :] = (gate_mix / (1.0 + jnp.exp(-gate_mix)) * value_mix).astype(BF)

    def pair_copy(k):
        return remote(pb.at[k, :, 1 - c], pr.at[k], dp_s.at[k], dp_r.at[k], peer)

    def rs_copy(k, d):
        zz = at_z(d)
        return remote(qq.at[k, zz], rb.at[at_z(k), z], rs_s.at[k, d], rs_r.at[at_z(k), z], {"sp": zz * m + r})

    order = (0, 1, 3, 2)
    for n, k in enumerate(order):
        if k > 0:
            diag(2, k)
        settle(2, k)
        part = nt(hid[...], ud[blk(at_z(k), m * rows), :]).astype(BF)
        pb[k] = part.reshape(b, 2, share, quarter)
        pair_copy(k).start()
        pair_copy(k).wait_recv()
        qq[k] = (pb[k, :, c].astype(F32) + pr[k].astype(F32)).astype(BF)
        for d in (2, 1, 3):
            rs_copy(k, d).start()

    for k in order:
        zz = at_z(k)
        total = qq[k, z].astype(F32)
        for d in range(1, b):
            src = at_z(d)
            remote(rb.at[zz, src], rb.at[zz, src], rs_s.at[k, d], rs_r.at[zz, src], {"sp": src * m + r}).wait_recv()
            total = total + rb[zz, src].astype(F32)
        cols = blk(zz, quarter)
        fb[c, :, cols] = (stream_ref[:, cols].astype(F32) + total).astype(BF)

    f_copy = remote(fb.at[c], fb.at[c], f_s, f_r, peer)
    f_copy.start()
    mine = pltpu.make_async_copy(fb.at[c], out_hbm.at[blk(c, share), :], loc.at[0])
    mine.start()
    remote(fb.at[1 - c], fb.at[1 - c], f_s, f_r, peer).wait_recv()
    other = pltpu.make_async_copy(fb.at[1 - c], out_hbm.at[blk(1 - c, share), :], loc.at[1])
    other.start()

    for k in range(1, count):
        note_copy(k).wait_send()
    for w in range(3):
        for k in range(b):
            if k > 0:
                z_copy(w, k).wait_send()
            for copy in near_copies(w, k):
                copy.wait_send()
            diag_copy(w, k).wait_send()
    for h in range(heads):
        s_copy(h).wait_send()
        t_copy(h).wait_send()

        @pl.when(z < b - 1)
        def _(h=h):
            e_copy(h).wait_send()
    a_copy.wait_send()
    tails.wait_send()
    f_copy.wait_send()
    for k in range(b):
        n_pass(k).wait_send()
        pair_copy(k).wait_send()
        if k > 0:
            n_copy(k).wait_send()
        for d in range(1, b):
            rs_copy(k, d).wait_send()
    mine.wait()
    other.wait()


def fused(residual, query_proj, key_proj, value_proj, out_gate, log_decay, doc_ids, head_gain,
          w_out, ffn_gain, w_gate, w_value, w_down_t, conv_taps, conv_bias):
    count = lax.axis_size("sp")
    rows = doc_ids.shape[0]
    heads = head_gain.shape[0]
    dk = query_proj.shape[1] // heads
    dv = value_proj.shape[1] // heads
    hidden_here = w_gate.shape[1]
    width = residual.shape[1]
    b = m = 4
    fc = hidden_here // b
    half, quarter = rows // 2, width // b
    vmem, dma = pltpu.VMEM, pltpu.SemaphoreType.DMA
    hbm = pl.BlockSpec(memory_space=pl.ANY)
    scratch = [
        vmem((rows, heads * dk), BF), vmem((rows, heads * dk), BF), vmem((rows, heads * dv), BF), vmem((rows, heads * dk), F32),
        vmem((rows, heads * dv), BF), vmem((half, width), BF), vmem((heads * dv, width), BF),
        vmem((width, 2 * fc), BF), vmem((width, fc), BF), vmem((rows, heads * dk), F32), vmem((count, 8, dk), F32),
        vmem((rows, heads * dk), BF), vmem((rows, heads * dv), F32),
        vmem((heads * dv, dk), BF), vmem((heads * dv, dk), BF), vmem((heads * dv, dk), BF), vmem((heads * dv, dk), BF),
        vmem((heads * dv, dk), BF), vmem((heads * dv, dk), BF), vmem((heads * dv, dk), F32),
        vmem((rows, width), F32), vmem((2, half, width), BF), vmem((half, width), BF), vmem((half, width), BF),
        vmem((b, 2, half, width), BF), vmem((b, rows + 8, 2 * fc), F32), vmem((2 * b, 2 * fc), F32), vmem((2 * b, 2 * fc), F32),
        vmem((2, b, rows, 1), F32), vmem((b * rows, fc), BF), vmem((b, b, 2, half, quarter), BF), vmem((b, b, half, quarter), BF),
        vmem((b, b, half, quarter), BF), vmem((b, b, half, quarter), BF), vmem((2, half, width), BF),
        dma((10,)), dma((count,)), dma((count,)), dma((3, b)), dma((3, count)), dma((3, b)), dma((3, b)), dma((3, b)),
        dma((heads,)), dma((heads,)), dma((heads,)), dma((heads,)), dma((heads,)), dma((heads,)), dma(()), dma(()),
        dma((b,)), dma((b,)), dma((b,)), dma((b,)), dma(()), dma(()), dma((b,)), dma((b,)), dma((b, b)), dma((b, b)), dma(()), dma(()),
    ]
    return pl.pallas_call(
        functools.partial(fused_kernel, (heads, dk, dv, rows, width, fc, count)),
        out_shape=jax.ShapeDtypeStruct((rows, width), BF),
        in_specs=[hbm] * 10 + [VMEM] * 5,
        out_specs=hbm,
        scratch_shapes=scratch,
        compiler_params=pltpu.CompilerParams(collective_id=0, has_side_effects=True, vmem_limit_bytes=56 * 2 ** 20),
    )(query_proj, key_proj, value_proj, log_decay, out_gate, residual, w_out, w_gate, w_value, w_down_t,
      doc_ids[None, :], head_gain, ffn_gain[None, :], conv_taps, conv_bias)


def one_kernel(count, tp, rows, heads, dk, dv, width, hidden_here):
    return (plane_count(count, hidden_here) == 4 and count == 16 and tp == 2 and rows == 128 and dk == rows
            and dv % 128 == 0 and heads <= 4 and width == count * rows)


def solution(mesh):
    placed = (
        P("sp", None), P("sp", "tp"), P("sp", "tp"), P("sp", "tp"), P("sp", "tp"), P("sp", "tp"),
        P("sp"), P("tp", None), P("tp", None), P(), P("sp", "tp"), P("sp", "tp"), P("sp", "tp"),
        P(None, None, "tp"), P(None, "tp"),
    )
    return jax.shard_map(per_device, mesh=mesh, in_specs=placed, out_specs=P("sp", None), check_vma=False)
```

```python
import functools

import jax
import jax.numpy as jnp
from jax import lax
from jax.experimental import pallas as pl
from jax.experimental.pallas import tpu as pltpu
from jax.sharding import PartitionSpec as P

EPS = 1e-06
VMEM = pl.BlockSpec(memory_space=pltpu.VMEM)
HIGH = lax.Precision.HIGHEST
BF = jnp.bfloat16
F32 = jnp.float32


def plane_count(positions, hidden):
    return max(b for b in (1, 2, 4) if positions % b == 0 and (hidden // b) % 128 == 0)


def nt(a, b):
    return lax.dot_general(a, b, (((1,), (1,)), ((), ())), preferred_element_type=F32)


def tn(a, b):
    return lax.dot_general(a, b, (((0,), (0,)), ((), ())), preferred_element_type=F32)


def local_kernel(heads, q_ref, k_ref, v_ref, g_ref, dcol_ref, drow_ref, o_ref, s_ref, qd_ref, cum_ref):
    rows = q_ref.shape[0]
    dk = q_ref.shape[1] // heads
    dv = v_ref.shape[1] // heads
    half = rows // 2
    t = lax.broadcasted_iota(jnp.int32, (rows, rows), 0)
    s = lax.broadcasted_iota(jnp.int32, (rows, rows), 1)
    tril = (t >= s).astype(F32)
    cum_ref[...] = jnp.dot(tril, g_ref[...], precision=HIGH, preferred_element_type=F32)
    dcol = dcol_ref[...]
    allowed = (t >= s) & (dcol == drow_ref[...])
    tail = (dcol == dcol_ref[rows - 1:rows, :]).astype(F32)
    scale = dk ** -0.5
    for h in range(heads):
        kc = pl.ds(h * dk, dk)
        vc = pl.ds(h * dv, dv)
        cum = cum_ref[:, kc]
        q = q_ref[:, kc].astype(F32) * scale
        k = k_ref[:, kc].astype(F32)
        v = v_ref[:, vc]
        total = cum[rows - 1:rows, :]
        qd_ref[:, kc] = (q * jnp.exp(cum)).astype(BF)
        s_ref[kc, :] = tn((k * jnp.exp(total - cum) * tail).astype(BF), v).astype(BF)
        edge = cum[half - 1:half, :]
        for part in range(2):
            rs = slice(part * half, (part + 1) * half)
            mid = cum[part * half + half // 2 - 1:part * half + half // 2, :]
            qs = (q[rs] * jnp.exp(cum[rs] - mid)).astype(BF)
            ks = (k[rs] * jnp.exp(mid - cum[rs])).astype(BF)
            a = jnp.where(allowed[rs, rs], nt(qs, ks), 0.0).astype(BF)
            o = jnp.dot(a, v[rs], preferred_element_type=F32)
            if part == 1:
                qx = (q[rs] * jnp.exp(cum[rs] - edge)).astype(BF)
                kx = (k[:half] * jnp.exp(edge - cum[:half])).astype(BF)
                x = jnp.where(allowed[rs, :half], nt(qx, kx), 0.0).astype(BF)
                o = o + jnp.dot(x, v[:half], preferred_element_type=F32)
            o_ref[rs, vc] = o


def out_kernel(heads, o_ref, qd_ref, p_ref, reach_ref, gate_ref, gain_ref, w_ref, out_ref, mixed):
    dk = qd_ref.shape[1] // heads
    dv = o_ref.shape[1] // heads
    for h in range(heads):
        kc = pl.ds(h * dk, dk)
        vc = pl.ds(h * dv, dv)
        carried = jnp.dot(qd_ref[:, kc], p_ref[kc, :], preferred_element_type=F32)
        head = o_ref[:, vc] + carried * reach_ref[...]
        head = head * lax.rsqrt(jnp.mean(head * head, axis=-1, keepdims=True) + EPS) * gain_ref[h:h + 1, :]
        gate = gate_ref[:, vc].astype(F32)
        mixed[:, vc] = (head * gate / (1.0 + jnp.exp(-gate))).astype(BF)
    out_ref[...] = jnp.dot(mixed[...], w_ref[...], preferred_element_type=F32).astype(BF)


def rotate(value, count, stride_in, size, steps):
    perm = []
    for i in range(count):
        d = (i // stride_in) % size
        perm.append((i, i + (((d + steps) % size) - d) * stride_in))
    return lax.ppermute(value, "sp", perm)


def swap(value):
    n = lax.axis_size("tp")
    return [lax.ppermute(value, "tp", [(i, (i + k) % n) for i in range(n)]) for k in range(1, n)]


def tp_gather(value):
    n = lax.axis_size("tp")
    if n != 2:
        return lax.all_gather(value, "tp", axis=0)
    (other,) = swap(value)
    first = lax.axis_index("tp") == 0
    return jnp.stack([jnp.where(first, value, other), jnp.where(first, other, value)])


def tp_scatter(value):
    n = lax.axis_size("tp")
    if n != 2:
        return lax.psum_scatter(value, "tp", scatter_dimension=0, tiled=False).astype(F32)
    c = lax.axis_index("tp")
    give = lax.dynamic_index_in_dim(value, 1 - c, 0, False)
    keep = lax.dynamic_index_in_dim(value, c, 0, False)
    return keep.astype(F32) + swap(give)[0].astype(F32)


def ordered(own, received, place, size):
    buf = jnp.zeros((size,) + own.shape, own.dtype)
    buf = lax.dynamic_update_index_in_dim(buf, own, place, 0)
    for k, item in enumerate(received, 1):
        buf = lax.dynamic_update_index_in_dim(buf, item, (place - k) % size, 0)
    return buf


def plane_gather(block, count, m, r, groups):
    b, depth, columns = block.shape
    if m != 4 or b % 2:
        got = lax.all_gather(block, "sp", axis=0, axis_index_groups=groups)
        return got.transpose(1, 0, 2, 3).reshape(b * m * depth, columns)
    half = b // 2
    near = rotate(block, count, 1, 2, 1)
    far = rotate(block, count, 2, 2, 1)
    diag_top = rotate(near[:half], count, 2, 2, 1)
    diag_low = rotate(far[half:], count, 1, 2, 1)
    x, y = r % 2, r // 2
    buf = jnp.zeros((b, m, depth, columns), block.dtype)

    def put(buf, item, first, i, j):
        return lax.dynamic_update_slice(buf, item[:, None], (first, 2 * j + i, 0, 0))

    buf = put(buf, block, 0, x, y)
    buf = put(buf, near, 0, 1 - x, y)
    buf = put(buf, far, 0, x, 1 - y)
    buf = put(buf, diag_top, 0, 1 - x, 1 - y)
    buf = put(buf, diag_low, half, 1 - x, 1 - y)
    return buf.reshape(b * m * depth, columns)


def per_device(residual, query_proj, key_proj, value_proj, out_gate, log_decay, doc_ids, head_gain,
               w_out, ffn_gain, w_gate, w_value, w_down_t, conv_taps, conv_bias):
    count = lax.axis_size("sp")
    rows = doc_ids.shape[0]
    heads = head_gain.shape[0]
    dk = query_proj.shape[1] // heads
    dv = value_proj.shape[1] // heads
    depth, hidden_here = w_gate.shape
    width = residual.shape[1]
    if one_kernel(count, lax.axis_size("tp"), rows, heads, dk, dv, width, hidden_here):
        return fused(residual, query_proj, key_proj, value_proj, out_gate, log_decay, doc_ids, head_gain,
                     w_out, ffn_gain, w_gate, w_value, w_down_t, conv_taps, conv_bias)
    b = plane_count(count, hidden_here)
    m = count // b
    fc = hidden_here // b
    place = lax.axis_index("sp")
    z, r = place // m, place % m
    groups = [[g * m + i for i in range(m)] for g in range(b)]

    note = jnp.concatenate([jnp.sum(log_decay, axis=0), doc_ids.astype(F32)])
    if b == 1:
        notes = lax.all_gather(note, "sp", axis=0)
    else:
        note = note[None]
        plane = ordered(note, [rotate(note, count, 1, m, k) for k in range(1, m)], r, m)
        notes = ordered(plane, [rotate(plane, count, m, b, k) for k in range(1, b)], z, b)
        notes = notes.reshape(count, -1)
    w_gate, w_value, notes = lax.optimization_barrier((w_gate, w_value, notes))

    def chunk(w, j):
        return lax.dynamic_slice_in_dim(w, j * fc, fc, 1)

    def exchange(pick):
        received = [rotate(pick((z + k) % b), count, m, b, k) for k in range(1, b)]
        block = ordered(pick(z), received, z, b)
        return plane_gather(block, count, m, r, groups)

    up_w = exchange(lambda j: jnp.concatenate([chunk(w_gate, j), chunk(w_value, j)], axis=1))

    totals, docs = notes[:, :heads * dk], notes[:, heads * dk:]
    first, last = docs[:, 0], docs[:, -1]
    steps = jnp.arange(count)

    o_local, state, q_dec = pl.pallas_call(
        functools.partial(local_kernel, heads),
        out_shape=(
            jax.ShapeDtypeStruct((rows, heads * dv), F32),
            jax.ShapeDtypeStruct((heads * dk, dv), BF),
            jax.ShapeDtypeStruct((rows, heads * dk), BF),
        ),
        in_specs=[VMEM] * 6,
        out_specs=(VMEM,) * 3,
        scratch_shapes=[pltpu.VMEM((rows, heads * dk), F32)],
        cost_estimate=pl.CostEstimate(flops=10**9, bytes_accessed=3 * 10**6, transcendentals=0),
    )(query_proj, key_proj, value_proj, log_decay, doc_ids[:, None], doc_ids[None, :])

    if b > 1:
        state, _ = lax.optimization_barrier((state, plane))

    def weight(source, until):
        inside = (steps > source) & (steps < until)
        return jnp.exp(jnp.sum(jnp.where(inside[:, None], totals, 0.0), axis=0))

    my_first = first[place]
    if b == 1:
        all_states = lax.all_gather(state, "sp", axis=0)

        def add(i, acc):
            live = (i < place) & (last[i] == my_first)
            scale = jnp.where(live, weight(i, place), 0.0)
            return acc + scale[:, None] * all_states[i].astype(F32)

        prefix = lax.fori_loop(0, count, add, jnp.zeros(state.shape, F32))
    else:
        near = [state] + [rotate(state, count, 1, m, k) for k in range(1, m)]
        end = (z + 1) * m
        start = z * m
        rows_of = []
        for k in range(1, m):
            source = start + (r - k) % m
            rows_of.append((source, place, (source < place) & (last[source] == my_first)))
        for k in range(m):
            source = start + (r - k) % m
            rows_of.append((source, end, last[source] == last[end - 1]))
        for k in range(1, b):
            source = jnp.maximum(z - k + 1, 0) * m - 1
            rows_of.append((source, start, (z >= k) & (last[source] == first[start])))
        rows_of.append((start - 1, place, first[start] == my_first))
        sources, untils, lives = (jnp.stack(col)[:, None] for col in zip(*rows_of))
        inside = ((steps > sources) & (steps < untils)).astype(F32)
        gaps = lax.dot_general(totals, inside, (((0,), (1,)), ((), ())), precision=HIGH,
                               preferred_element_type=F32)
        scales = jnp.where(lives[:, 0], jnp.exp(jnp.minimum(gaps, 0.0)), 0.0)
        pick_scale = lambda i: scales[:, i:i + 1]
        prefix = sum(pick_scale(k - 1) * near[k].astype(F32) for k in range(1, m))
        plane_end = sum(pick_scale(m - 1 + k) * near[k].astype(F32) for k in range(m)).astype(BF)
        whole = sum(
            pick_scale(2 * m - 2 + k)
            * lax.ppermute(plane_end, "sp", [(i, i + k * m) for i in range(count - k * m)]).astype(F32)
            for k in range(1, b)
        )
        prefix += pick_scale(2 * m - 2 + b) * whole

    prefix = prefix.astype(BF)
    w_down_t, prefix = lax.optimization_barrier((w_down_t, prefix))
    down_w = exchange(lambda j: chunk(w_down_t, j))

    own_docs = doc_ids.astype(F32)
    prev_last = jnp.where(place > 0, last[place - 1], -1.0)
    reach_rows = ((own_docs == my_first) & (prev_last == my_first)).astype(F32)[:, None]
    attn = pl.pallas_call(
        functools.partial(out_kernel, heads),
        out_shape=jax.ShapeDtypeStruct((rows, width), BF),
        in_specs=[VMEM] * 7,
        out_specs=VMEM,
        scratch_shapes=[pltpu.VMEM((rows, heads * dv), BF)],
        cost_estimate=pl.CostEstimate(flops=10**9, bytes_accessed=6 * 10**6, transcendentals=0),
    )(o_local, q_dec, prefix, reach_rows, out_gate, head_gain, w_out)

    tp = lax.axis_size("tp")
    share = rows // tp
    core = lax.axis_index("tp")
    attn_sum = tp_scatter(attn.reshape(tp, share, width))
    own_rows = lax.dynamic_slice_in_dim(residual, core * share, share, 0)
    stream = (own_rows.astype(F32) + attn_sum).astype(BF)
    stream_f = stream.astype(F32)
    normed = (stream_f * lax.rsqrt(jnp.mean(stream_f * stream_f, axis=-1, keepdims=True) + EPS) * ffn_gain).astype(BF)
    blocks = ordered(normed, [rotate(normed, count, m, b, k) for k in range(1, b)], z, b)
    full = tp_gather(blocks).transpose(1, 0, 2, 3).reshape(b * rows, width)
    ups = jnp.dot(full, up_w, preferred_element_type=F32).astype(BF).reshape(b, rows, 2 * fc)

    tails = rotate(ups[:, -2:], count, 1, m, 1)
    lead = jnp.where(r == 0, jnp.roll(tails, 1, axis=0), tails)
    ext = jnp.concatenate([lead, ups], axis=1).astype(F32)
    at = jnp.arange(b) * m + r
    block_docs = docs[at]
    prev = jnp.where((at > 0)[:, None], docs[(at - 1) % count][:, -2:], -1.0)
    doc_ext = jnp.concatenate([prev, block_docs], axis=1)
    one = (doc_ext[:, 1:-1] == block_docs).astype(F32)[:, :, None]
    two = (doc_ext[:, :-2] == block_docs).astype(F32)[:, :, None]
    taps = lax.dynamic_slice_in_dim(conv_taps, z * fc, fc, 2).reshape(3, 2 * fc)
    bias = lax.dynamic_slice_in_dim(conv_bias, z * fc, fc, 1).reshape(2 * fc)
    mix = bias + taps[2] * ext[:, 2:] + taps[1] * ext[:, 1:-1] * one + taps[0] * ext[:, :-2] * two
    gate_mix, value_mix = mix[..., :fc], mix[..., fc:]
    hidden = (jax.nn.silu(gate_mix) * value_mix).astype(BF).reshape(b * rows, fc)
    partial = nt(hidden, down_w).astype(BF)

    partial = partial.reshape(b, tp, share, width).transpose(1, 0, 2, 3)
    pair = tp_scatter(partial).astype(BF)
    total = lax.dynamic_index_in_dim(pair, z, 0, False).astype(F32)
    for k in range(1, b):
        total += rotate(lax.dynamic_index_in_dim(pair, (z + k) % b, 0, False), count, m, b, k).astype(F32)
    finished = (stream_f + total).astype(BF)
    return tp_gather(finished).reshape(rows, width)


MESH = pl.DeviceIdType.MESH


ORDER = (0, 1, 3, 2)
PLAN = {
    (0, 0): ("s12", "s02"),
    (0, 1): ("s00", "n11", "d01", "s10", "s02", "n21", "s13"),
    (0, 2): ("s13", "s23", "s11", "n12", "n03", "n10"),
    (0, 3): ("s02", "s01", "s00", "s11", "s10", "s12"),
    (1, 0): ("s11", "n11"),
    (1, 1): ("s03", "n12", "n10"),
    (1, 2): ("s21", "s10", "s03", "n00", "n01"),
    (1, 3): ("n13", "n12", "n22", "n02", "n01", "n11", "n23"),
    (2, 0): ("s01", "d00", "n01", "n10", "n20", "d11", "d01", "d10", "s03", "n03"),
    (2, 1): ("s12",),
    (2, 2): ("s01", "n22", "d03", "d00", "n13", "d02"),
    (2, 3): ("d01",),
    (3, 0): ("s13", "n13", "n12", "n21"),
    (3, 1): ("d11", "d12", "n13", "d10", "s20", "d13", "n03"),
    (3, 2): ("s00", "n11", "d10", "d12"),
    (3, 3): ("d02", "d03", "d13"),
    (4, 0): ("n02", "d12", "d13", "s21", "s23", "t2", "s22", "d02", "d03", "t1", "t3", "d21"),
    (4, 1): ("n02", "n00", "d03", "d21", "t0", "t2", "d02", "d00", "t3"),
    (4, 2): ("d22", "d13", "t1", "t3", "d11", "d01", "t0", "n23"),
    (4, 3): ("n00", "s22", "n10", "t2", "d12", "d22", "d11", "t1", "d23", "d00", "d10", "n20", "s20", "t0", "s21"),
    (5, 0): ("d20",),
    (5, 1): ("n22", "s22"),
    (5, 2): ("s20",),
    (6, 0): ("n22",),
    (6, 1): ("n20", "s23"),
    (6, 2): ("d23",),
    (6, 3): ("d20",),
    (7, 0): ("n23",),
    (7, 1): ("d22",),
    (7, 2): ("n21",),
    (7, 3): ("n21",),
    (8, 1): ("d20",),
    (10, 0): ("d22",),
    (10, 1): ("n23",),
    (10, 3): ("d21",),
    (11, 0): ("d23",),
    (11, 2): ("n20", "d21"),
    (12, 1): ("d23",),
    (12, 2): ("d20",),
}


def fused_kernel(cfg, q_hbm, k_hbm, v_hbm, g_hbm, gate_hbm, res_hbm, wo_hbm, wg_hbm, wv_hbm, wd_hbm,
                 doc_ref, gain_ref, fgain_ref, taps_ref, bias_ref, out_hbm,
                 qb, kb, vb, gb, gateb, resb, wo, ugv, ud, cum_ref, notes, qd, o_ref, s_own, s_x, t2, s_y, e_in, e_out, pref,
                 acc, a_own, a_peer, stream_ref, nf, ups, tail_s, tail_r, masks, hid, pb, pr, qq, rb, fb,
                 loc, n_s, n_r, wz_s, w_r, wx_s, wy_s, wd_s, sx_s, sx_r, sy_s, sy_r, sz_s, sz_r, ap_s, ap_r,
                 nz_s, nz_r, nd_s, nd_r, tl_s, tl_r, dp_s, dp_r, rs_s, rs_r, f_s, f_r):
    heads, dk, dv, rows, width, fc, count = cfg
    b = m = 4
    half, share, quarter = rows // 2, rows // 2, width // b
    hbm_w = (wg_hbm, wv_hbm, wd_hbm)
    p, c = lax.axis_index("sp"), lax.axis_index("tp")
    z, r = lax.div(p, m), lax.rem(p, m)
    x, y = lax.rem(r, 2), lax.div(r, 2)
    xr, yr = r + 1 - 2 * x, r + 2 - 4 * y
    xn, yn, base = z * m + xr, z * m + yr, z * m
    peer = {"tp": 1 - c}

    def remote(src, dst, ss, rs, dev):
        return pltpu.make_async_remote_copy(src_ref=src, dst_ref=dst, send_sem=ss, recv_sem=rs, device_id=dev,
                                            device_id_type=MESH)

    def at_z(k):
        return lax.rem(z + k, b)

    def blk(i, n):
        return pl.ds(pl.multiple_of(i * n, n), n)

    def w_at(w, i):
        if w == 2:
            return ud.at[blk(i, rows), :]
        return ugv.at[blk(i, rows), pl.ds(w * fc, fc)]

    def w_from(w, zz):
        return hbm_w[w].at[:, pl.ds(pl.multiple_of(zz * fc, 128), fc)]

    local = [pltpu.make_async_copy(src, dst, loc.at[i]) for i, (src, dst) in enumerate([
        (g_hbm, gb), (k_hbm, kb), (v_hbm, vb), (q_hbm, qb), (gate_hbm, gateb),
        (res_hbm.at[blk(c, share), :], resb), (wo_hbm, wo),
        (w_from(0, z), w_at(0, p)), (w_from(1, z), w_at(1, p)), (w_from(2, z), w_at(2, p))])]
    for copy in local:
        copy.start()

    barrier = pltpu.get_barrier_semaphore()
    for k in range(1, count):
        pl.semaphore_signal(barrier, inc=1, device_id={"sp": lax.rem(p + k, count)}, device_id_type=MESH)
    pl.semaphore_signal(barrier, inc=1, device_id=peer, device_id_type=MESH)

    ti = lax.broadcasted_iota(jnp.int32, (rows, rows), 0)
    si = lax.broadcasted_iota(jnp.int32, (rows, rows), 1)
    lower, same = ti >= si, ti == si

    def column(row):
        return jnp.sum(jnp.where(same, row, 0.0), axis=1, keepdims=True)

    drow = doc_ref[...].astype(F32)
    dcol = column(drow)
    allowed = lower & (dcol == drow)
    last_doc = drow[:, rows - 1:rows]
    tail = (dcol == last_doc).astype(F32)
    tril = lower.astype(F32).astype(BF)

    local[0].wait()
    decay = gb[...]
    d1 = decay.astype(BF)
    rest = decay - d1.astype(F32)
    d2 = rest.astype(BF)
    d3 = (rest - d2.astype(F32)).astype(BF)
    dot = functools.partial(jnp.dot, preferred_element_type=F32)
    cum_ref[...] = dot(tril, d1) + (dot(tril, d2) + dot(tril, d3))
    for h in range(heads):
        notes[p, h:h + 1, :] = cum_ref[rows - 1:rows, h * dk:(h + 1) * dk]
    for h in range(heads, 4):
        notes[p, h:h + 1, :] = jnp.zeros((1, dk), F32)
    notes[p, 4:5, :] = drow
    notes[p, 5:6, :] = drow
    notes[p, 6:7, :] = jnp.broadcast_to(last_doc, (1, rows))
    notes[p, 7:8, :] = drow

    @pl.when(z == 0)
    def _():
        e_in[...] = jnp.zeros_like(e_in)

    pl.semaphore_wait(barrier, count)

    def note_copy(k):
        to = lax.rem(p + k, count)
        return remote(notes.at[p], notes.at[p], n_s.at[k], n_r.at[p], {"sp": to})

    for k in range(1, count):
        note_copy(k).start()

    def z_copy(w, k):
        zz = at_z(k)
        return remote(w_from(w, zz), w_at(w, p), wz_s.at[w, k], w_r.at[w, p], {"sp": zz * m + r})

    def near_copies(w, k):
        i = at_z(k) * m + r
        src = w_from(w, z) if k == 0 else w_at(w, i)
        return (remote(src, w_at(w, i), wx_s.at[w, k], w_r.at[w, i], {"sp": xn}),
                remote(src, w_at(w, i), wy_s.at[w, k], w_r.at[w, i], {"sp": yn}))

    def diag_copy(w, k):
        zs = at_z(k)
        even = lax.rem(zs, 2) == 0
        i = zs * m + jnp.where(even, xr, yr)
        return remote(w_at(w, i), w_at(w, i), wd_s.at[w, k], w_r.at[w, i], {"sp": jnp.where(even, yn, xn)})

    def arrived(w, i):
        remote(w_at(w, i), w_at(w, i), wx_s.at[w, 0], w_r.at[w, i], {"sp": xn}).wait_recv()

    def near(w, k):
        if k > 0:
            arrived(w, at_z(k) * m + r)
        for copy in near_copies(w, k):
            copy.start()

    def diag(w, k):
        zs = at_z(k)
        arrived(w, zs * m + jnp.where(lax.rem(zs, 2) == 0, xr, yr))
        diag_copy(w, k).start()

    def n_copy(i, up):
        to = jnp.minimum(p + m, count - m + r) if up else jnp.maximum(p - m, r)
        return remote(nf.at[i, c], nf.at[i, c], nz_s.at[int(up), i], nz_r.at[i], {"sp": to})

    def n_pass(i):
        return remote(nf.at[i, c], nf.at[i, c], nd_s.at[i], nd_r.at[i], peer)

    def act(plane, kind, *at):
        k = (at[-1] - plane) % b
        if kind == "s":
            z_copy(at[0], k).start()
        elif kind == "n":
            near(at[0], k)
        elif kind == "d":
            diag(at[0], k)
        else:
            i, up = at[0], at[0] < plane
            n_copy(i, up).wait_recv()
            if plane < b - 1 if up else plane > 0:
                n_copy(i, up).start()
            n_pass(i).start()

    def run(slot):
        for plane in range(b):
            steps = PLAN.get((slot, plane), ())
            if steps:
                @pl.when(z == plane)
                def _(plane=plane, steps=steps):
                    for step in steps:
                        act(plane, step[0], *map(int, step[1:]))

    def settle(w, k):
        zs = at_z(k)
        arrived(w, zs * m + jnp.where(lax.rem(zs, 2) == 0, yr, xr))
        arrived(w, zs * m + 3 - r)

    near_g = near_copies(0, 0)
    near_g[1].start()

    local[1].wait()
    local[2].wait()

    def s_copy(h):
        return remote(s_own.at[blk(h, dv), :], s_x.at[blk(h, dv), :], sx_s.at[h], sx_r.at[h], {"sp": xn})

    def t_copy(h):
        return remote(t2.at[blk(h, dv), :], s_y.at[blk(h, dv), :], sy_s.at[h], sy_r.at[h], {"sp": yn})

    def e_copy(h):
        return remote(e_out.at[blk(h, dv), :], e_in.at[blk(h, dv), :], sz_s.at[h], sz_r.at[h],
                      {"sp": jnp.minimum(p + m, count - m + r)})

    for h in range(heads):
        kc, vc = slice(h * dk, (h + 1) * dk), slice(h * dv, (h + 1) * dv)
        cum = cum_ref[:, kc]
        k_end = (kb[:, kc].astype(F32) * jnp.exp(cum[rows - 1:rows, :] - cum) * tail).astype(BF)
        s_own[vc, :] = tn(vb[:, vc], k_end).astype(BF)
        s_copy(h).start()
    near_g[0].start()
    local[3].wait()
    scale = dk ** -0.5
    for h in range(heads):
        kc, vc = slice(h * dk, (h + 1) * dk), slice(h * dv, (h + 1) * dv)
        cum = cum_ref[:, kc]
        q = qb[:, kc].astype(F32) * scale
        k = kb[:, kc].astype(F32)
        v = vb[:, vc]
        qd[:, kc] = (q * jnp.exp(cum)).astype(BF)
        edge = cum[half - 1:half, :]
        for part in range(2):
            rs = slice(part * half, (part + 1) * half)
            mid = cum[part * half + half // 2 - 1:part * half + half // 2, :]
            qs = (q[rs] * jnp.exp(cum[rs] - mid)).astype(BF)
            ks = (k[rs] * jnp.exp(mid - cum[rs])).astype(BF)
            own = jnp.sum(q[rs] * k[rs], axis=1, keepdims=True)
            a = jnp.where(same[rs, rs], own, jnp.where(allowed[rs, rs], nt(qs, ks), 0.0)).astype(BF)
            o = dot(a, v[rs])
            if part == 1:
                qx = (q[rs] * jnp.exp(cum[rs] - edge)).astype(BF)
                kx = (k[:half] * jnp.exp(edge - cum[:half])).astype(BF)
                cross = jnp.where(allowed[rs, :half], nt(qx, kx), 0.0).astype(BF)
                o = o + dot(cross, v[:half])
            o_ref[rs, vc] = o

    run(0)

    def note_from(i):
        remote(notes.at[i], notes.at[i], n_s.at[0], n_r.at[i], {"sp": i}).wait_recv()

    note_from(xn)

    def last_of(i):
        return notes[i, 6:7, :]

    def weight(source, until, live):
        total = jnp.zeros((8, dk), F32)
        for s in range(count):
            total = total + jnp.where((s > source) & (s < until), notes[s], 0.0)
        total = jnp.exp(jnp.minimum(total, 0.0))
        return jnp.where(live, total, 0.0)

    before = jnp.maximum(p - 1, 0)
    plane_before = jnp.maximum(base - 1, 0)
    pair = p - x
    w_pair = jnp.where(last_of(pair) == last_of(pair + 1), jnp.exp(jnp.minimum(notes[pair + 1], 0.0)), 0.0)

    for h in range(heads):
        vc = slice(h * dv, (h + 1) * dv)
        s_copy(h).wait_recv()
        own, got = s_own[vc, :].astype(F32), s_x[vc, :].astype(F32)
        left = jnp.where(x == 0, own, got)
        right = jnp.where(x == 0, got, own)
        t2[vc, :] = (right + left * w_pair[h:h + 1, :]).astype(BF)
        t_copy(h).start()
        pref[vc, :] = jnp.where(x == 1, got, 0.0)

    note_from(yn)
    note_from(base + 3 - r)
    for k in range(1, b):
        for i in range(m):
            note_from(at_z(k) * m + i)
    w_plane = weight(base + 1, base + m, last_of(base + 1) == last_of(base + 3))
    w_line = weight(base - 1, base + m, (last_of(plane_before) == last_of(base + 3)) & (z > 0))
    w_py = weight(base + 1, p, (last_of(base + 1) == last_of(before)) & (y == 1))
    w_pz = weight(base - 1, p, (last_of(plane_before) == last_of(before)) & (z > 0))
    reach = ((dcol == column(jnp.broadcast_to(notes[before, 6:7, :], (rows, rows)))) & (p > 0)).astype(F32)

    for copy in local[4:]:
        copy.wait()
    run(1)

    for h in range(heads):
        kc, vc = slice(h * dk, (h + 1) * dk), slice(h * dv, (h + 1) * dv)
        t_copy(h).wait_recv()
        own, got = t2[vc, :].astype(F32), s_y[vc, :].astype(F32)
        left = jnp.where(y == 0, own, got)
        right = jnp.where(y == 0, got, own)
        plane = right + left * w_plane[h:h + 1, :]

        @pl.when(z > 0)
        def _(h=h):
            e_copy(h).wait_recv()
        enter = e_in[vc, :].astype(F32)
        e_out[vc, :] = (plane + enter * w_line[h:h + 1, :]).astype(BF)

        @pl.when(z < b - 1)
        def _(h=h):
            e_copy(h).start()
        prefix = pref[vc, :] + got * w_py[h:h + 1, :] + enter * w_pz[h:h + 1, :]
        carried = nt(qd[:, kc], prefix.astype(BF))
        head = o_ref[:, vc] + carried * reach
        head = head * lax.rsqrt(jnp.mean(head * head, axis=-1, keepdims=True) + EPS) * gain_ref[h:h + 1, :]
        gate = gateb[:, vc].astype(F32)
        mixed = (head * gate / (1.0 + jnp.exp(-gate))).astype(BF)
        if h == 0:
            acc[...] = dot(mixed, wo[vc, :])
        else:
            acc[...] += dot(mixed, wo[vc, :])
    run(2)

    a_own[0] = acc[0:share, :].astype(BF)
    a_own[1] = acc[share:rows, :].astype(BF)
    a_copy = remote(a_own.at[1 - c], a_peer, ap_s, ap_r, peer)
    a_copy.start()
    run(3)

    for zb in range(b):
        at = zb * m + r
        row = notes[at, 4:5, :]
        prow = jnp.where(at > 0, notes[jnp.maximum(at - 1, 0), 4:5, :], -1.0)
        lane = lax.broadcasted_iota(jnp.int32, (1, rows), 1)
        for lag in (1, 2):
            shifted = jnp.where(lane < lag, pltpu.roll(prow, lag, 1), pltpu.roll(row, lag, 1))
            masks[lag - 1, zb] = column((shifted == row).astype(F32))

    a_copy.wait_recv()
    stream = (resb[...].astype(F32) + (a_own[c].astype(F32) + a_peer[...].astype(F32))).astype(BF)
    stream_ref[...] = stream
    stream_f = stream.astype(F32)
    normed = (stream_f * lax.rsqrt(jnp.mean(stream_f * stream_f, axis=-1, keepdims=True) + EPS) * fgain_ref[...]).astype(BF)
    nf[z, c] = normed

    @pl.when(z < b - 1)
    def _():
        n_copy(z, True).start()

    @pl.when(z > 0)
    def _():
        n_copy(z, False).start()
    n_pass(z).start()

    run(4)

    for k in range(b):
        zz = at_z(k)
        remote(nf.at[zz, 1 - c], nf.at[zz, 1 - c], nd_s.at[zz], nd_r.at[zz], peer).wait_recv()
    for k in range(b):
        settle(0, k)
    for k in range(b):
        settle(1, k)
    run(5)

    lanes = 256 if (2 * fc) % 256 == 0 else 128

    @pl.loop(0, 2 * fc // lanes)
    def _(j):
        cs = pl.ds(pl.multiple_of(j * lanes, lanes), lanes)
        full = nf[...].reshape(b * rows, width)
        up = dot(full, ugv[:, cs]).astype(BF).astype(F32)
        for zb in range(b):
            ups[zb, 8:8 + rows, cs] = up[zb * rows:(zb + 1) * rows]
            tail_s[2 * zb:2 * zb + 2, cs] = up[(zb + 1) * rows - 2:(zb + 1) * rows]

    tails = remote(tail_s, tail_r, tl_s, tl_r, {"sp": base + lax.rem(r + 1, m)})
    tails.start()
    run(6)
    tails.wait_recv()
    got = tail_r[...]
    for zb in range(b):
        prev = (zb - 1) % b
        ups[zb, 6:8, :] = jnp.where(r == 0, got[2 * prev:2 * prev + 2], got[2 * zb:2 * zb + 2])

    off = pl.multiple_of(z * fc, 128)
    taps = [taps_ref[i, :, pl.ds(off, fc)] for i in range(3)]
    bias = bias_ref[:, pl.ds(off, fc)]

    @pl.loop(0, b)
    def _(zb):
        one, two = masks[0, zb], masks[1, zb]

        def mix(w):
            cols = slice(w * fc, (w + 1) * fc)
            t = [tap[w:w + 1] for tap in taps]
            return (bias[w:w + 1] + t[2] * ups[zb, 8:8 + rows, cols] + t[1] * ups[zb, 7:7 + rows, cols] * one
                    + t[0] * ups[zb, 6:6 + rows, cols] * two)

        gate_mix, value_mix = mix(0), mix(1)
        hid[blk(zb, rows), :] = (gate_mix / (1.0 + jnp.exp(-gate_mix)) * value_mix).astype(BF)

    def pair_copy(k):
        return remote(pb.at[k, :, 1 - c], pr.at[k], dp_s.at[k], dp_r.at[k], peer)

    def rs_copy(k, d):
        zz = at_z(d)
        return remote(qq.at[k, zz], rb.at[at_z(k), z], rs_s.at[k, d], rs_r.at[at_z(k), z], {"sp": zz * m + r})

    def down(k):
        settle(2, k)
        part = nt(hid[...], ud[blk(at_z(k), m * rows), :]).astype(BF)
        pb[k] = part.reshape(b, 2, share, quarter)
        pair_copy(k).start()

    def scatter(k):
        pair_copy(k).wait_recv()
        qq[k] = (pb[k, :, c].astype(F32) + pr[k].astype(F32)).astype(BF)
        for d in (2, 1, 3):
            rs_copy(k, d).start()

    run(7)
    down(ORDER[0])
    run(8)
    scatter(ORDER[0])
    run(9)
    down(ORDER[1])
    run(10)
    scatter(ORDER[1])
    run(11)
    down(ORDER[2])
    run(12)
    scatter(ORDER[2])
    run(13)
    down(ORDER[3])
    run(14)
    scatter(ORDER[3])
    run(15)

    for k in ORDER:
        zz = at_z(k)
        total = qq[k, z].astype(F32)
        for d in range(1, b):
            src = at_z(d)
            remote(rb.at[zz, src], rb.at[zz, src], rs_s.at[k, d], rs_r.at[zz, src], {"sp": src * m + r}).wait_recv()
            total = total + rb[zz, src].astype(F32)
        cols = blk(zz, quarter)
        fb[c, :, cols] = (stream_ref[:, cols].astype(F32) + total).astype(BF)

    f_copy = remote(fb.at[c], fb.at[c], f_s, f_r, peer)
    f_copy.start()
    mine = pltpu.make_async_copy(fb.at[c], out_hbm.at[blk(c, share), :], loc.at[0])
    mine.start()
    remote(fb.at[1 - c], fb.at[1 - c], f_s, f_r, peer).wait_recv()
    other = pltpu.make_async_copy(fb.at[1 - c], out_hbm.at[blk(1 - c, share), :], loc.at[1])
    other.start()

    for k in range(1, count):
        note_copy(k).wait_send()
    for w in range(3):
        for k in range(b):
            if k > 0:
                z_copy(w, k).wait_send()
            for copy in near_copies(w, k):
                copy.wait_send()
            diag_copy(w, k).wait_send()
    for h in range(heads):
        s_copy(h).wait_send()
        t_copy(h).wait_send()

        @pl.when(z < b - 1)
        def _(h=h):
            e_copy(h).wait_send()
    a_copy.wait_send()
    tails.wait_send()
    f_copy.wait_send()
    for k in range(b):
        n_pass(k).wait_send()
        pair_copy(k).wait_send()

        @pl.when((k <= z) & (z < b - 1))
        def _(k=k):
            n_copy(k, True).wait_send()

        @pl.when((k >= z) & (z > 0))
        def _(k=k):
            n_copy(k, False).wait_send()
        for d in range(1, b):
            rs_copy(k, d).wait_send()
    mine.wait()
    other.wait()


def fused(residual, query_proj, key_proj, value_proj, out_gate, log_decay, doc_ids, head_gain,
          w_out, ffn_gain, w_gate, w_value, w_down_t, conv_taps, conv_bias):
    count = lax.axis_size("sp")
    rows = doc_ids.shape[0]
    heads = head_gain.shape[0]
    dk = query_proj.shape[1] // heads
    dv = value_proj.shape[1] // heads
    hidden_here = w_gate.shape[1]
    width = residual.shape[1]
    b = m = 4
    fc = hidden_here // b
    half, quarter = rows // 2, width // b
    vmem, dma = pltpu.VMEM, pltpu.SemaphoreType.DMA
    hbm = pl.BlockSpec(memory_space=pl.ANY)
    scratch = [
        vmem((rows, heads * dk), BF), vmem((rows, heads * dk), BF), vmem((rows, heads * dv), BF), vmem((rows, heads * dk), F32),
        vmem((rows, heads * dv), BF), vmem((half, width), BF), vmem((heads * dv, width), BF),
        vmem((width, 2 * fc), BF), vmem((width, fc), BF), vmem((rows, heads * dk), F32), vmem((count, 8, dk), F32),
        vmem((rows, heads * dk), BF), vmem((rows, heads * dv), F32),
        vmem((heads * dv, dk), BF), vmem((heads * dv, dk), BF), vmem((heads * dv, dk), BF), vmem((heads * dv, dk), BF),
        vmem((heads * dv, dk), BF), vmem((heads * dv, dk), BF), vmem((heads * dv, dk), F32),
        vmem((rows, width), F32), vmem((2, half, width), BF), vmem((half, width), BF), vmem((half, width), BF),
        vmem((b, 2, half, width), BF), vmem((b, rows + 8, 2 * fc), F32), vmem((2 * b, 2 * fc), F32), vmem((2 * b, 2 * fc), F32),
        vmem((2, b, rows, 1), F32), vmem((b * rows, fc), BF), vmem((b, b, 2, half, quarter), BF), vmem((b, b, half, quarter), BF),
        vmem((b, b, half, quarter), BF), vmem((b, b, half, quarter), BF), vmem((2, half, width), BF),
        dma((10,)), dma((count,)), dma((count,)), dma((3, b)), dma((3, count)), dma((3, b)), dma((3, b)), dma((3, b)),
        dma((heads,)), dma((heads,)), dma((heads,)), dma((heads,)), dma((heads,)), dma((heads,)), dma(()), dma(()),
        dma((2, b)), dma((b,)), dma((b,)), dma((b,)), dma(()), dma(()), dma((b,)), dma((b,)), dma((b, b)), dma((b, b)), dma(()), dma(()),
    ]
    return pl.pallas_call(
        functools.partial(fused_kernel, (heads, dk, dv, rows, width, fc, count)),
        out_shape=jax.ShapeDtypeStruct((rows, width), BF),
        in_specs=[hbm] * 10 + [VMEM] * 5,
        out_specs=hbm,
        scratch_shapes=scratch,
        compiler_params=pltpu.CompilerParams(collective_id=0, has_side_effects=True, vmem_limit_bytes=56 * 2 ** 20),
    )(query_proj, key_proj, value_proj, log_decay, out_gate, residual, w_out, w_gate, w_value, w_down_t,
      doc_ids[None, :], head_gain, ffn_gain[None, :], conv_taps, conv_bias)


def one_kernel(count, tp, rows, heads, dk, dv, width, hidden_here):
    return (plane_count(count, hidden_here) == 4 and count == 16 and tp == 2 and rows == 128 and dk == rows
            and dv % 128 == 0 and heads <= 4 and width == count * rows)


def solution(mesh):
    placed = (
        P("sp", None), P("sp", "tp"), P("sp", "tp"), P("sp", "tp"), P("sp", "tp"), P("sp", "tp"),
        P("sp"), P("tp", None), P("tp", None), P(), P("sp", "tp"), P("sp", "tp"), P("sp", "tp"),
        P(None, None, "tp"), P(None, "tp"),
    )
    return jax.shard_map(per_device, mesh=mesh, in_specs=placed, out_specs=P("sp", None), check_vma=False)
```
